32 devices in a mesh: sp: 8 (over z, y), tp: 4 (over x, core).
Axes of the slice: x: 2, y: 2, z: 4, core: 2. Of those that a mesh axis runs over, the one named last changes fastest.
Arguments:
- inputs: bfloat16 [8192, 2048], P(('sp', 'tp')), may hold values from -90 to 90
- in_gain: float32 [2048], replicated, may hold values from 0.1 to 1.9
- w_query: bfloat16 [2048, 1024], replicated, may hold values from -2 to 2
- w_key: bfloat16 [2048, 128], replicated, may hold values from -2 to 2
- w_value: bfloat16 [2048, 128], replicated, may hold values from -0.125 to 0.125
- query_gain: float32 [64], replicated, may hold values from 0 to 8, as said below
- key_gain: float32 [64], replicated, may hold values from 0 to 8, as said below
- decay_sums: float32 [8192, 16], P('sp', 'tp'), may hold values from -1173 to 0, as said below
- w_out: bfloat16 [1024, 2048], replicated, may hold values from -0.1875 to 0.1875
Outputs:
- result: bfloat16 [8192, 2048], P(('sp', 'tp'))
The draws below stay inside these ranges and needn't reach their ends.
Inputs may be any that keep to these rules, and one draw needn't show every extreme that they name: `decay_sums`: along positions, each head's entries never rise. `query_gain`: every entry is positive. `key_gain`: every entry is positive.
All inputs are finite; a program needn't handle non-finite values.
Results may differ from the reference program's by a relative error of at most 0.015.
The reference program's roundings to bfloat16 on the way count: a program that leaves them out, or rounds other values in their place, can miss the bound.
Values may be sent and summed in bfloat16 or wider, within the bound.
A program may use at most 64 MiB of HBM per device.

```python
import math
import jax
import jax.numpy as jnp
from jax import lax

D = 2048
QUERY_HEADS = 16
DH = 64
KV = 2
TOK_DEV = 1024
SEQUENCE_LENGTH = 8192


def draw_inputs(key, part):
    key_noise, key_shift = jax.random.split(jax.random.fold_in(key, 13), 2)
    noise = jax.random.truncated_normal(key_noise, -5.0, 5.0, (SEQUENCE_LENGTH, D), jnp.float32)
    shift = jax.random.truncated_normal(key_shift, -4.0, 4.0, (SEQUENCE_LENGTH // TOK_DEV, D), jnp.float32)
    shifted = noise + jnp.repeat(shift, TOK_DEV, axis=0)
    return shifted.astype(jnp.bfloat16)


def draw_w_query(key, part):
    noise = jax.random.truncated_normal(jax.random.fold_in(key, 31), -6.0, 6.0, (D, QUERY_HEADS * DH), jnp.float32) * D ** (-0.5)
    return noise.astype(jnp.bfloat16)


def draw_w_key(key, part):
    noise = jax.random.truncated_normal(jax.random.fold_in(key, 32), -6.0, 6.0, (D, KV * DH), jnp.float32) * D ** (-0.5)
    return noise.astype(jnp.bfloat16)


def draw_query_gain(key, part):
    return jax.random.uniform(jax.random.fold_in(key, 11), (DH,), jnp.float32, 0.4, 1.6)


def draw_key_gain(key, part):
    return jax.random.uniform(jax.random.fold_in(key, 12), (DH,), jnp.float32, 0.4, 1.6)


def draw_decay_sums(key, part):
    random_part_keys = jax.random.split(jax.random.fold_in(key, 14), 7)
    order = jax.random.permutation(random_part_keys[0], QUERY_HEADS)
    fast_count = QUERY_HEADS // 2
    fast = (order < fast_count)[None, :]
    slow_rate = jax.random.uniform(random_part_keys[1], (1, QUERY_HEADS), jnp.float32, 0.2, 0.6) / SEQUENCE_LENGTH
    fast_rate = jax.random.uniform(random_part_keys[2], (1, QUERY_HEADS), jnp.float32, 1.0 / 60.0, 1.0 / 25.0)
    base_offset = jnp.where(fast, fast_rate, slow_rate)
    coarse_estimate = jax.random.uniform(random_part_keys[3], (SEQUENCE_LENGTH, QUERY_HEADS), jnp.float32, 0.3, 1.7)
    block_multiple = jnp.exp(jax.random.uniform(random_part_keys[4], (SEQUENCE_LENGTH // TOK_DEV, QUERY_HEADS), jnp.float32, -math.log(2.0), math.log(2.0)))
    block_multiple = jnp.repeat(block_multiple, TOK_DEV, axis=0)
    spike_position = jax.random.randint(random_part_keys[5], (3,), 0, SEQUENCE_LENGTH)
    spike_depth = jnp.log(jax.random.uniform(random_part_keys[6], (3, QUERY_HEADS), jnp.float32, 0.5, 0.8))
    match_count = (jnp.arange(SEQUENCE_LENGTH, dtype=jnp.int32)[:, None] == spike_position[None, :]).astype(jnp.float32)
    spike_list = jnp.dot(match_count, spike_depth, precision=lax.Precision.HIGHEST)
    step_log_gates = -base_offset * coarse_estimate * block_multiple + spike_list
    return jnp.cumsum(step_log_gates, axis=0)


def gaussian(rng, shape, spread, most, kind=jnp.bfloat16):
    drawn = jax.random.normal(rng, shape, jnp.float32) * spread
    return jnp.minimum(jnp.maximum(drawn, -most), most).astype(kind)


def setup_inputs(seed: int = 0) -> dict:
    arg_keys = jax.random.split(jax.random.key(seed), 10)
    inputs = draw_inputs(jax.random.fold_in(arg_keys[9], 71), 0)
    in_gain = jnp.clip(1.0 + 0.18 * jax.random.normal(arg_keys[1], (D,), jnp.float32), 0.1, 1.9)
    w_query = draw_w_query(jax.random.fold_in(arg_keys[9], 71), 0)
    w_key = draw_w_key(jax.random.fold_in(arg_keys[9], 71), 0)
    w_value = gaussian(arg_keys[4], (D, KV * DH), D ** -0.5, 0.125)
    query_gain = draw_query_gain(jax.random.fold_in(arg_keys[9], 71), 0)
    key_gain = draw_key_gain(jax.random.fold_in(arg_keys[9], 71), 0)
    decay_sums = draw_decay_sums(jax.random.fold_in(arg_keys[9], 71), 0)
    w_out = gaussian(arg_keys[8], (QUERY_HEADS * DH, D), (QUERY_HEADS * DH) ** -0.5, 0.1875)
    return dict(inputs=inputs, in_gain=in_gain, w_query=w_query, w_key=w_key, w_value=w_value, query_gain=query_gain, key_gain=key_gain, decay_sums=decay_sums, w_out=w_out)


epsilon = 1e-06

def rms_norm(vector, gain_vec):
    return vector * lax.rsqrt(lax.optimization_barrier(jnp.mean(vector * vector, axis=-1, keepdims=True)) + epsilon) * gain_vec

def reference(inputs, in_gain, w_query, w_key, w_value, query_gain, key_gain, decay_sums, w_out):
    length = inputs.shape[0]
    normed = rms_norm(inputs.astype(jnp.float32), in_gain).astype(jnp.bfloat16)
    queries = rms_norm(jnp.dot(normed, w_query, preferred_element_type=jnp.float32).reshape(length, QUERY_HEADS, DH), query_gain).astype(jnp.bfloat16)
    keys = rms_norm(jnp.dot(normed, w_key, preferred_element_type=jnp.float32).reshape(length, KV, DH), key_gain).astype(jnp.bfloat16)
    values = jnp.dot(normed, w_value, preferred_element_type=jnp.float32).astype(jnp.bfloat16).reshape(length, KV, DH)
    group_size = QUERY_HEADS // KV
    keys_wide = jnp.repeat(keys, group_size, axis=1).astype(jnp.float32)
    values_wide = jnp.repeat(values, group_size, axis=1).astype(jnp.float32)
    block_rows = math.gcd(length, 512)
    block_count = length // block_rows
    key_pos = jnp.arange(length, dtype=jnp.int32)
    key_decay = decay_sums.T
    score_scale = DH ** (-0.5)

    def attend_block(block_index):
        offset = (block_index * block_rows).astype(jnp.int32)
        query_rows = lax.dynamic_slice_in_dim(queries, offset, block_rows, 0).astype(jnp.float32)
        query_decay = lax.dynamic_slice_in_dim(decay_sums, offset, block_rows, 0)
        scores = jnp.einsum('qhd,khd->hqk', query_rows, keys_wide) * score_scale
        scores = scores + query_decay.T[:, :, None] - key_decay[:, None, :]
        query_pos = offset + jnp.arange(block_rows, dtype=jnp.int32)
        visible = key_pos[None, :] <= query_pos[:, None]
        scores = jnp.where(visible[None], scores, -1e+30)
        peak = lax.optimization_barrier(jnp.max(scores, axis=-1, keepdims=True))
        weights_exp = jnp.where(visible[None], jnp.exp(scores - peak), 0.0)
        total = lax.optimization_barrier(jnp.sum(weights_exp, axis=-1))
        rounded = lax.optimization_barrier(weights_exp.astype(jnp.bfloat16)).astype(jnp.float32)
        mixed = jnp.einsum('hqk,khd->qhd', rounded, values_wide)
        return (mixed / total.T[:, :, None]).astype(jnp.bfloat16)
    blocks = lax.map(attend_block, jnp.arange(block_count, dtype=jnp.int32))
    attended = blocks.reshape(length, QUERY_HEADS * DH)
    return jnp.dot(attended, w_out, preferred_element_type=jnp.float32).astype(jnp.bfloat16)
```

```python
import math

import jax
import jax.numpy as jnp
from jax import lax
from jax.experimental import pallas as pl
from jax.experimental.pallas import tpu as pltpu
from jax.sharding import Mesh, PartitionSpec as P

epsilon = 1e-06
LOG2E = math.log2(math.e)
ALL = ("sp", "kv", "half")
HEADS_PER_DOT = 2


def rms_norm(vector, gain_vec):
    return (
        vector * lax.rsqrt(jnp.mean(vector * vector, axis=-1, keepdims=True) + epsilon) * gain_vec
    )


def attend_kernel(
    place_ref, queries_ref, decay_ref, packed_ref, out_ref, kv_ref, ones_ref, q_ref, peak_ref,
    acc_ref, sems, *, rows, heads, half_count, tp_count, key_block
):
    members = packed_ref.shape[0]
    blocks = 2 * members
    group = place_ref[2]
    copies = []
    for j in range(members):
        block = (j // half_count) * tp_count + group * half_count + j % half_count
        for part, where in ((0, block), (1, blocks - 1 - block)):
            copies.append(
                pltpu.make_async_copy(
                    packed_ref.at[j, pl.ds(part * rows, rows)],
                    kv_ref.at[pl.ds(pl.multiple_of(where * rows, rows), rows)],
                    sems.at[2 * j + part],
                )
            )
            copies[-1].start()
    lane = lax.broadcasted_iota(jnp.int32, (rows, 128), 1)
    low = lane < 64
    for r in range(2):
        for pair in range(heads // 2):
            both = queries_ref[r, :, pair * 128 : (pair + 1) * 128].astype(jnp.float32)
            even = jnp.where(low, both, 0.0)
            odd = jnp.where(low, pltpu.roll(both, 64, 1), 0.0)
            q_ref[r, (2 * pair) * rows : (2 * pair + 1) * rows] = even.astype(jnp.bfloat16)
            q_ref[r, (2 * pair + 1) * rows : (2 * pair + 2) * rows] = odd.astype(jnp.bfloat16)
    for copy in copies:
        copy.wait()

    def fill(i, carry):
        at = pl.ds(pl.multiple_of(i * key_block, key_block), key_block)
        wide = lax.broadcasted_iota(jnp.int32, (key_block, 128), 1) < 64
        ones_ref[at] = jnp.where(wide, 1.0, kv_ref[at].astype(jnp.float32)).astype(jnp.bfloat16)
        return carry

    lax.fori_loop(0, kv_ref.shape[0] // key_block, fill, 0)
    span = HEADS_PER_DOT * rows

    for r in range(2):
        first = place_ref[r]
        peak_ref[...] = jnp.full_like(peak_ref, -1e30)
        acc_ref[...] = jnp.zeros_like(acc_ref)

        def step(index, masked):
            at = pl.ds(pl.multiple_of(index * key_block, key_block), key_block)
            keys = kv_ref[at]
            values = ones_ref[at]
            for start in range(0, heads, HEADS_PER_DOT):
                part = pl.ds(start * rows, span)
                scores = lax.dot_general(
                    q_ref[r, part], keys, (((1,), (1,)), ((), ())),
                    preferred_element_type=jnp.float32,
                )
                scores = scores.reshape(HEADS_PER_DOT, rows, key_block)
                scores = scores - decay_ref[index, start : start + HEADS_PER_DOT][:, None, :]
                if masked:
                    row = first + lax.broadcasted_iota(jnp.int32, (rows, key_block), 0)
                    col = index * key_block + lax.broadcasted_iota(
                        jnp.int32, (rows, key_block), 1
                    )
                    scores = jnp.where((col <= row)[None], scores, -1e30)
                scores = scores.reshape(span, key_block)
                before = peak_ref[part]
                after = jnp.maximum(before, jnp.max(scores, axis=1, keepdims=True))
                weights = jnp.exp2(scores - after[:, :1]).astype(jnp.bfloat16)
                acc_ref[part] = acc_ref[part] * jnp.exp2(before - after) + jnp.dot(
                    weights, values, preferred_element_type=jnp.float32
                )
                peak_ref[part] = after

        full = first // key_block

        def body(index, carry):
            step(index, False)
            return carry

        lax.fori_loop(0, full, body, 0)
        step(full, True)
        for pair in range(heads // 2):
            even = acc_ref[(2 * pair) * rows : (2 * pair + 1) * rows]
            odd = acc_ref[(2 * pair + 1) * rows : (2 * pair + 2) * rows]
            done = jnp.where(low, pltpu.roll(even, 64, 1), odd) / jnp.where(
                low, even, pltpu.roll(odd, 64, 1)
            )
            out_ref[r, :, pair * 128 : (pair + 1) * 128] = done.astype(jnp.bfloat16)


def per_device(inputs, in_gain, w_query, w_key, w_value, query_gain, key_gain, decay_sums, w_out):
    sp_count = lax.axis_size("sp")
    kv_heads = lax.axis_size("kv")
    half_count = lax.axis_size("half")
    tp_count = kv_heads * half_count
    group = lax.axis_index("kv")
    me = (lax.axis_index("sp") * kv_heads + group) * half_count + lax.axis_index("half")
    count = sp_count * tp_count
    mirror = [(i, count - 1 - i) for i in range(count)]
    head_size = query_gain.shape[0]
    rows = inputs.shape[0]
    length = rows * count
    all_heads = w_query.shape[1] // head_size
    heads = all_heads // kv_heads
    width = heads * head_size
    members = sp_count * half_count
    key_block = math.gcd(length, 512)

    def choose(a, b):
        return jnp.where(group == 0, a, b)

    normed = rms_norm(inputs.astype(jnp.float32), in_gain).astype(jnp.bfloat16)
    keys = rms_norm(
        jnp.dot(normed, w_key, preferred_element_type=jnp.float32).reshape(
            rows, kv_heads, head_size
        ),
        key_gain,
    ).astype(jnp.bfloat16)
    values = (
        jnp.dot(normed, w_value, preferred_element_type=jnp.float32)
        .astype(jnp.bfloat16)
        .reshape(rows, kv_heads, head_size)
    )
    pairs = jnp.concatenate([keys, values], axis=2)
    own_kv = choose(pairs[:, 0], pairs[:, 1])
    far_kv = lax.ppermute(choose(pairs[:, 1], pairs[:, 0]), ALL, mirror)

    decays = decay_sums.T * LOG2E
    high = lax.reduce_precision(decays, 8, 7)
    rest = decays - high
    middle = lax.reduce_precision(rest, 8, 7)
    pieces = jnp.stack([high, middle, rest - middle]).astype(jnp.bfloat16)
    packed = jnp.concatenate([own_kv, far_kv, pieces.reshape(-1, 128)], axis=0)
    gathered = lax.all_gather(packed, ("sp", "half"), axis=0, tiled=False)

    queries = rms_norm(
        jnp.dot(normed, w_query, preferred_element_type=jnp.float32).reshape(
            rows, all_heads, head_size
        ),
        query_gain * (LOG2E * head_size ** (-0.5)),
    ).astype(jnp.bfloat16).reshape(rows, kv_heads * width)
    own_q = choose(queries[:, :width], queries[:, width:])
    far_q = lax.ppermute(choose(queries[:, width:], queries[:, :width]), ALL, mirror)

    decay_all = jnp.sum(
        gathered[:, 2 * rows :].reshape(sp_count, half_count, 3, -1, 128).astype(jnp.float32),
        axis=2,
    ).reshape(sp_count, heads, -1, key_block)
    decay_all = decay_all.transpose(0, 2, 1, 3).reshape(length // key_block, heads, key_block)
    place = jnp.stack([me * rows, (count - 1 - me) * rows, group]).astype(jnp.int32)
    vmem = pl.BlockSpec(memory_space=pltpu.VMEM)
    attended = pl.pallas_call(
        lambda *refs: attend_kernel(
            *refs, rows=rows, heads=heads, half_count=half_count, tp_count=tp_count,
            key_block=key_block,
        ),
        out_shape=jax.ShapeDtypeStruct((2, rows, width), jnp.bfloat16),
        in_specs=[
            pl.BlockSpec(memory_space=pltpu.SMEM), vmem, vmem, pl.BlockSpec(memory_space=pl.ANY)
        ],
        out_specs=vmem,
        scratch_shapes=[
            pltpu.VMEM((length, 128), jnp.bfloat16),
            pltpu.VMEM((length, 128), jnp.bfloat16),
            pltpu.VMEM((2, heads * rows, 128), jnp.bfloat16),
            pltpu.VMEM((heads * rows, 128), jnp.float32),
            pltpu.VMEM((heads * rows, 128), jnp.float32),
            pltpu.SemaphoreType.DMA((2 * members,)),
        ],
        compiler_params=pltpu.CompilerParams(vmem_limit_bytes=48 * 1024 * 1024),
        name="attend",
    )(place, jnp.stack([own_q, far_q]), decay_all, gathered)
    back = lax.ppermute(attended[1], ALL, mirror)
    whole = choose(
        jnp.concatenate([attended[0], back], axis=1), jnp.concatenate([back, attended[0]], axis=1)
    )
    return jnp.dot(whole, w_out, preferred_element_type=jnp.float32).astype(jnp.bfloat16)


def solution(mesh):
    sp_count, tp_count = mesh.devices.shape
    split = Mesh(mesh.devices.reshape(sp_count, 2, tp_count // 2), ALL)
    placed = (P(ALL, None), P(), P(), P(), P(), P(), P(), P("sp", ("kv", "half")), P())
    return jax.shard_map(
        per_device, mesh=split, in_specs=placed, out_specs=P(ALL, None), check_vma=False
    )
```

```python
import math

import jax
import jax.numpy as jnp
from jax import lax
from jax.experimental import pallas as pl
from jax.experimental.pallas import tpu as pltpu
from jax.sharding import Mesh, PartitionSpec as P

epsilon = 1e-06
LOG2E = math.log2(math.e)
ALL = ("sp", "kv", "half")
HEADS_PER_DOT = 2
KEY_BLOCK = 512
SMALL = 60.0


def rms_norm(vector, gain_vec):
    return (
        vector * lax.rsqrt(jnp.mean(vector * vector, axis=-1, keepdims=True) + epsilon) * gain_vec
    )


def exchange_kernel(
    kv_ref, q_ref, decay_ref, kv_out, q_out, decay_out, own_sems, kv_send, kv_recv, kv_relay,
    decay_send, decay_recv, decay_relay, q_send, q_recv, *, rows, sizes
):
    sp_count, kv_heads, half_count = sizes
    sp, group, half = lax.axis_index("sp"), lax.axis_index("kv"), lax.axis_index("half")
    core, chips = half % 2, half_count // 2
    partner = (sp, group, half + 1 - 2 * core)

    def device_of(chip):
        return (chip // (kv_heads * chips), (chip // chips) % kv_heads, (chip % chips) * 2 + core)

    def block_of(place):
        return (place[0] * kv_heads + place[1]) * half_count + place[2]

    def kv_copy(source, block, send, device):
        return pltpu.make_async_remote_copy(
            src_ref=source, dst_ref=kv_out.at[pl.ds(pl.multiple_of(block * rows, rows), rows)],
            send_sem=send, recv_sem=kv_recv.at[block], device_id=device,
            device_id_type=pl.DeviceIdType.MESH,
        )

    def decay_copy(source, member, send, device):
        return pltpu.make_async_remote_copy(
            src_ref=source, dst_ref=decay_out.at[member], send_sem=send,
            recv_sem=decay_recv.at[member], device_id=device,
            device_id_type=pl.DeviceIdType.MESH,
        )

    me = block_of((sp, group, half))
    chip = (sp * kv_heads + group) * chips + half // 2
    total = sp_count * kv_heads * chips
    member = sp * half_count + half
    cluster = sp * chips + half // 2
    clusters = sp_count * chips
    started = []
    for k in range(1, total):
        place = device_of((chip + k) % total)
        started.append(kv_copy(kv_ref.at[place[1]], me, kv_send.at[k], place))
        started[-1].start()
    for k in range(1, clusters):
        other = (cluster + k) % clusters
        place = (other // chips, group, (other % chips) * 2 + core)
        started.append(decay_copy(decay_ref, member, decay_send.at[k], place))
        started[-1].start()
    q_copy = pltpu.make_async_remote_copy(
        src_ref=q_ref, dst_ref=q_out, send_sem=q_send, recv_sem=q_recv,
        device_id=(sp_count - 1 - sp, kv_heads - 1 - group, half_count - 1 - half),
        device_id_type=pl.DeviceIdType.MESH,
    )
    q_copy.start()
    started.append(kv_copy(kv_ref.at[group], me, kv_relay.at[0], partner))
    started[-1].start()
    started.append(decay_copy(decay_ref, member, decay_relay.at[0], partner))
    started[-1].start()
    own_kv = pltpu.make_async_copy(
        kv_ref.at[group], kv_out.at[pl.ds(pl.multiple_of(me * rows, rows), rows)], own_sems.at[0]
    )
    own_kv.start()
    own_decay = pltpu.make_async_copy(decay_ref, decay_out.at[member], own_sems.at[1])
    own_decay.start()
    for k in range(1, clusters):
        other = (cluster + clusters - k) % clusters
        which = (other // chips) * half_count + (other % chips) * 2 + core
        landed = decay_out.at[which]
        relay = decay_copy(landed, which, decay_relay.at[k], partner)
        relay.wait_recv()
        relay.start()
        started.append(relay)
    for k in range(1, total):
        block = block_of(device_of((chip + total - k) % total))
        landed = kv_out.at[pl.ds(pl.multiple_of(block * rows, rows), rows)]
        relay = kv_copy(landed, block, kv_relay.at[k], partner)
        relay.wait_recv()
        relay.start()
        started.append(relay)
    for k in range(clusters):
        other = (cluster + clusters - k) % clusters
        which = (other // chips) * half_count + (other % chips) * 2 + 1 - core
        decay_copy(decay_out.at[which], which, decay_relay.at[k], partner).wait_recv()
    for k in range(total):
        place = device_of((chip + total - k) % total)
        block = block_of((place[0], place[1], place[2] + 1 - 2 * core))
        landed = kv_out.at[pl.ds(pl.multiple_of(block * rows, rows), rows)]
        kv_copy(landed, block, kv_relay.at[k], partner).wait_recv()
    for copy in started:
        copy.wait_send()
    own_kv.wait()
    own_decay.wait()
    q_copy.wait()


def attend_kernel(
    place_ref, near_ref, far_ref, row_ref, decay_ref, kv_ref, out_ref, ones_ref, q_ref, peak_ref,
    acc_ref, *, rows, heads, key_block, small
):
    lane = lax.broadcasted_iota(jnp.int32, (rows, 128), 1)
    low = lane < 64
    for r, ref in enumerate((near_ref, far_ref)):
        for pair in range(heads // 2):
            both = ref[:, pair * 128 : (pair + 1) * 128].astype(jnp.float32)
            even = jnp.where(low, both, 0.0)
            odd = jnp.where(low, pltpu.roll(both, 64, 1), 0.0)
            q_ref[r, (2 * pair) * rows : (2 * pair + 1) * rows] = even.astype(jnp.bfloat16)
            q_ref[r, (2 * pair + 1) * rows : (2 * pair + 2) * rows] = odd.astype(jnp.bfloat16)

    def fill(i, carry):
        at = pl.ds(pl.multiple_of(i * key_block, key_block), key_block)
        wide = lax.broadcasted_iota(jnp.int32, (key_block, 128), 1) < 64
        ones_ref[at] = jnp.where(wide, 1.0, kv_ref[at].astype(jnp.float32)).astype(jnp.bfloat16)
        return carry

    lax.fori_loop(0, kv_ref.shape[0] // key_block, fill, 0)
    span = HEADS_PER_DOT * rows

    for r in range(2):
        first = place_ref[r]
        for head in range(heads):
            part = pl.ds(head * rows, rows)
            if small:
                peak_ref[part] = jnp.broadcast_to(row_ref[r, :, head : head + 1], (rows, 128))
            else:
                peak_ref[part] = jnp.full((rows, 128), -1e30, jnp.float32)
        acc_ref[...] = jnp.zeros_like(acc_ref)

        def step(index, masked):
            at = pl.ds(pl.multiple_of(index * key_block, key_block), key_block)
            keys = kv_ref[at]
            values = ones_ref[at]
            for start in range(0, heads, HEADS_PER_DOT):
                part = pl.ds(start * rows, span)
                before = peak_ref[part]
                scores = lax.dot_general(
                    q_ref[r, part], keys, (((1,), (1,)), ((), ())),
                    preferred_element_type=jnp.float32,
                )
                if small:
                    scores = scores + jnp.concatenate([before] * (key_block // 128), axis=1)
                scores = scores.reshape(HEADS_PER_DOT, rows, key_block)
                scores = scores - decay_ref[index, start : start + HEADS_PER_DOT][:, None, :]
                if masked:
                    row = first + lax.broadcasted_iota(jnp.int32, (rows, key_block), 0)
                    col = index * key_block + lax.broadcasted_iota(
                        jnp.int32, (rows, key_block), 1
                    )
                    scores = jnp.where((col <= row)[None], scores, -1e30)
                scores = scores.reshape(span, key_block)
                if small:
                    weights = jnp.exp2(scores).astype(jnp.bfloat16)
                    acc_ref[part] += jnp.dot(weights, values, preferred_element_type=jnp.float32)
                else:
                    after = jnp.maximum(before, jnp.max(scores, axis=1, keepdims=True))
                    weights = jnp.exp2(scores - after[:, :1]).astype(jnp.bfloat16)
                    acc_ref[part] = acc_ref[part] * jnp.exp2(before - after) + jnp.dot(
                        weights, values, preferred_element_type=jnp.float32
                    )
                    peak_ref[part] = after

        full = first // key_block

        def body(index, carry):
            step(index, False)
            return carry

        lax.fori_loop(0, full, body, 0)
        step(full, True)
        for pair in range(heads // 2):
            even = acc_ref[(2 * pair) * rows : (2 * pair + 1) * rows]
            odd = acc_ref[(2 * pair + 1) * rows : (2 * pair + 2) * rows]
            done = jnp.where(low, pltpu.roll(even, 64, 1), odd) / jnp.where(
                low, even, pltpu.roll(odd, 64, 1)
            )
            out_ref[r, :, pair * 128 : (pair + 1) * 128] = done.astype(jnp.bfloat16)


def attend(place, near, far, row_decay, decays, kv, small):
    length = kv.shape[0]
    rows, width = near.shape
    heads, key_block = decays.shape[1:]
    vmem = pl.BlockSpec(memory_space=pltpu.VMEM)
    return pl.pallas_call(
        lambda *refs: attend_kernel(
            *refs, rows=rows, heads=heads, key_block=key_block, small=small
        ),
        out_shape=jax.ShapeDtypeStruct((2, rows, width), jnp.bfloat16),
        in_specs=[pl.BlockSpec(memory_space=pltpu.SMEM)] + [vmem] * 5,
        out_specs=vmem,
        scratch_shapes=[
            pltpu.VMEM((length, 128), jnp.bfloat16),
            pltpu.VMEM((2, heads * rows, 128), jnp.bfloat16),
            pltpu.VMEM((heads * rows, 128), jnp.float32),
            pltpu.VMEM((heads * rows, 128), jnp.float32),
        ],
        compiler_params=pltpu.CompilerParams(vmem_limit_bytes=40 * 1024 * 1024),
        name="attend_small" if small else "attend_any",
    )(place, near, far, row_decay, decays, kv)


def per_device(inputs, in_gain, w_query, w_key, w_value, query_gain, key_gain, decay_sums, w_out):
    sp_count = lax.axis_size("sp")
    kv_heads = lax.axis_size("kv")
    half_count = lax.axis_size("half")
    tp_count = kv_heads * half_count
    group = lax.axis_index("kv")
    me = (lax.axis_index("sp") * kv_heads + group) * half_count + lax.axis_index("half")
    count = sp_count * tp_count
    mirror = [(i, count - 1 - i) for i in range(count)]
    head_size = query_gain.shape[0]
    rows = inputs.shape[0]
    length = rows * count
    all_heads = w_query.shape[1] // head_size
    heads = all_heads // kv_heads
    width = heads * head_size
    members = sp_count * half_count
    key_block = math.gcd(length, KEY_BLOCK)

    def choose(a, b):
        return jnp.where(group == 0, a, b)

    normed = rms_norm(inputs.astype(jnp.float32), in_gain).astype(jnp.bfloat16)
    keys = rms_norm(
        jnp.dot(normed, w_key, preferred_element_type=jnp.float32).reshape(
            rows, kv_heads, head_size
        ),
        key_gain,
    ).astype(jnp.bfloat16)
    values = (
        jnp.dot(normed, w_value, preferred_element_type=jnp.float32)
        .astype(jnp.bfloat16)
        .reshape(rows, kv_heads, head_size)
    )
    pairs = jnp.concatenate([keys, values], axis=2)
    kv_blocks = pairs.transpose(1, 0, 2)
    decay_rows = (decay_sums.T * LOG2E).reshape(-1, 128)

    queries = rms_norm(
        jnp.dot(normed, w_query, preferred_element_type=jnp.float32).reshape(
            rows, all_heads, head_size
        ),
        query_gain * (LOG2E * head_size ** (-0.5)),
    ).astype(jnp.bfloat16).reshape(rows, kv_heads * width)
    own_q = choose(queries[:, :width], queries[:, width:])
    sent_q = choose(queries[:, width:], queries[:, :width])
    vmem = pl.BlockSpec(memory_space=pltpu.VMEM)
    chips = count // 2
    dma = pltpu.SemaphoreType.DMA
    kv, far_q, decay_all = pl.pallas_call(
        lambda *refs: exchange_kernel(
            *refs, rows=rows, sizes=(sp_count, kv_heads, half_count)
        ),
        out_shape=(
            jax.ShapeDtypeStruct((length, 128), jnp.bfloat16),
            jax.ShapeDtypeStruct((rows, width), jnp.bfloat16),
            jax.ShapeDtypeStruct((members, *decay_rows.shape), jnp.float32),
        ),
        in_specs=[vmem] * 3,
        out_specs=(vmem,) * 3,
        scratch_shapes=[
            dma((2,)), dma((chips,)), dma((count,)), dma((chips,)), dma((members // 2,)),
            dma((members,)), dma((members // 2,)), dma, dma,
        ],
        compiler_params=pltpu.CompilerParams(has_side_effects=True),
        name="exchange",
    )(kv_blocks, sent_q, decay_rows)
    decay_all = decay_all.reshape(sp_count, heads, -1, key_block)
    decay_all = decay_all.transpose(0, 2, 1, 3).reshape(length // key_block, heads, key_block)
    firsts = (me * rows, (count - 1 - me) * rows)
    place = jnp.stack(firsts).astype(jnp.int32)
    row_decay = jnp.stack(
        [
            lax.dynamic_slice(
                decay_all, (first // key_block, 0, first % key_block), (1, heads, rows)
            )[0].T
            for first in firsts
        ]
    )
    bound = head_size**0.5 * LOG2E * jnp.max(query_gain) * jnp.max(key_gain)
    attended = lax.cond(
        bound <= SMALL,
        lambda *given: attend(*given, True),
        lambda *given: attend(*given, False),
        place, own_q, far_q, row_decay, decay_all, kv,
    )
    back = lax.ppermute(attended[1], ALL, mirror)
    whole = choose(
        jnp.concatenate([attended[0], back], axis=1), jnp.concatenate([back, attended[0]], axis=1)
    )
    return jnp.dot(whole, w_out, preferred_element_type=jnp.float32).astype(jnp.bfloat16)


def solution(mesh):
    sp_count, tp_count = mesh.devices.shape
    split = Mesh(mesh.devices.reshape(sp_count, 2, tp_count // 2), ALL)
    placed = (P(ALL, None), P(), P(), P(), P(), P(), P(), P("sp", ("kv", "half")), P())
    return jax.shard_map(
        per_device, mesh=split, in_specs=placed, out_specs=P(ALL, None), check_vma=False
    )
```

```python
import math

import jax
import jax.numpy as jnp
from jax import lax
from jax.experimental import pallas as pl
from jax.experimental.pallas import tpu as pltpu
from jax.sharding import Mesh, PartitionSpec as P

epsilon = 1e-06
LOG2E = math.log2(math.e)
ALL = ("sp", "kv", "half")
HEADS_PER_DOT = 2
KEY_BLOCK = 512
SMALL = 60.0


def rms_norm(vector, gain_vec):
    return (
        vector * lax.rsqrt(jnp.mean(vector * vector, axis=-1, keepdims=True) + epsilon) * gain_vec
    )


def exchange_kernel(
    kv_ref, q_ref, decay_ref, kv_out, q_out, decay_out, own_sems, kv_send, kv_recv, kv_relay,
    decay_send, decay_recv, decay_relay, q_send, q_recv, *, rows, sizes
):
    sp_count, kv_heads, half_count = sizes
    sp, group, half = lax.axis_index("sp"), lax.axis_index("kv"), lax.axis_index("half")
    core, chips = half % 2, half_count // 2
    partner = (sp, group, half + 1 - 2 * core)

    def device_of(chip):
        return (chip // (kv_heads * chips), (chip // chips) % kv_heads, (chip % chips) * 2 + core)

    def block_of(place):
        return (place[0] * kv_heads + place[1]) * half_count + place[2]

    def kv_copy(source, block, send, device):
        return pltpu.make_async_remote_copy(
            src_ref=source, dst_ref=kv_out.at[pl.ds(pl.multiple_of(block * rows, rows), rows)],
            send_sem=send, recv_sem=kv_recv.at[block], device_id=device,
            device_id_type=pl.DeviceIdType.MESH,
        )

    def decay_copy(source, member, send, device):
        return pltpu.make_async_remote_copy(
            src_ref=source, dst_ref=decay_out.at[member], send_sem=send,
            recv_sem=decay_recv.at[member], device_id=device,
            device_id_type=pl.DeviceIdType.MESH,
        )

    me = block_of((sp, group, half))
    chip = (sp * kv_heads + group) * chips + half // 2
    total = sp_count * kv_heads * chips
    member = sp * half_count + half
    cluster = sp * chips + half // 2
    clusters = sp_count * chips
    started = []
    for k in range(1, total):
        place = device_of((chip + k) % total)
        started.append(kv_copy(kv_ref.at[place[1]], me, kv_send.at[k], place))
        started[-1].start()
    for k in range(1, clusters):
        other = (cluster + k) % clusters
        place = (other // chips, group, (other % chips) * 2 + core)
        started.append(decay_copy(decay_ref, member, decay_send.at[k], place))
        started[-1].start()
    q_copy = pltpu.make_async_remote_copy(
        src_ref=q_ref, dst_ref=q_out, send_sem=q_send, recv_sem=q_recv,
        device_id=(sp_count - 1 - sp, kv_heads - 1 - group, half_count - 1 - half),
        device_id_type=pl.DeviceIdType.MESH,
    )
    q_copy.start()
    started.append(kv_copy(kv_ref.at[group], me, kv_relay.at[0], partner))
    started[-1].start()
    started.append(decay_copy(decay_ref, member, decay_relay.at[0], partner))
    started[-1].start()
    own_kv = pltpu.make_async_copy(
        kv_ref.at[group], kv_out.at[pl.ds(pl.multiple_of(me * rows, rows), rows)], own_sems.at[0]
    )
    own_kv.start()
    own_decay = pltpu.make_async_copy(decay_ref, decay_out.at[member], own_sems.at[1])
    own_decay.start()
    for k in range(1, clusters):
        other = (cluster + clusters - k) % clusters
        which = (other // chips) * half_count + (other % chips) * 2 + core
        landed = decay_out.at[which]
        relay = decay_copy(landed, which, decay_relay.at[k], partner)
        relay.wait_recv()
        relay.start()
        started.append(relay)
    for k in range(1, total):
        block = block_of(device_of((chip + total - k) % total))
        landed = kv_out.at[pl.ds(pl.multiple_of(block * rows, rows), rows)]
        relay = kv_copy(landed, block, kv_relay.at[k], partner)
        relay.wait_recv()
        relay.start()
        started.append(relay)
    for k in range(clusters):
        other = (cluster + clusters - k) % clusters
        which = (other // chips) * half_count + (other % chips) * 2 + 1 - core
        decay_copy(decay_out.at[which], which, decay_relay.at[k], partner).wait_recv()
    for k in range(total):
        place = device_of((chip + total - k) % total)
        block = block_of((place[0], place[1], place[2] + 1 - 2 * core))
        landed = kv_out.at[pl.ds(pl.multiple_of(block * rows, rows), rows)]
        kv_copy(landed, block, kv_relay.at[k], partner).wait_recv()
    for copy in started:
        copy.wait_send()
    own_kv.wait()
    own_decay.wait()
    q_copy.wait()


def attend_kernel(
    place_ref, near_ref, far_ref, row_ref, decay_ref, kv_ref, out_ref, ones_ref, q_ref, peak_ref,
    acc_ref, *, rows, heads, key_block, small
):
    lane = lax.broadcasted_iota(jnp.int32, (rows, 128), 1)
    low = lane < 64
    for r, ref in enumerate((near_ref, far_ref)):
        for pair in range(heads // 2):
            both = ref[:, pair * 128 : (pair + 1) * 128].astype(jnp.float32)
            even = jnp.where(low, both, 0.0)
            odd = jnp.where(low, pltpu.roll(both, 64, 1), 0.0)
            q_ref[r, (2 * pair) * rows : (2 * pair + 1) * rows] = even.astype(jnp.bfloat16)
            q_ref[r, (2 * pair + 1) * rows : (2 * pair + 2) * rows] = odd.astype(jnp.bfloat16)

    def fill(i, carry):
        at = pl.ds(pl.multiple_of(i * key_block, key_block), key_block)
        wide = lax.broadcasted_iota(jnp.int32, (key_block, 128), 1) < 64
        ones_ref[at] = jnp.where(wide, 1.0, kv_ref[at].astype(jnp.float32)).astype(jnp.bfloat16)
        return carry

    lax.fori_loop(0, kv_ref.shape[0] // key_block, fill, 0)
    span = HEADS_PER_DOT * rows

    for r in range(2):
        first = place_ref[r]
        for head in range(heads):
            part = pl.ds(head * rows, rows)
            if small:
                peak_ref[part] = jnp.broadcast_to(row_ref[r, :, head : head + 1], (rows, 128))
            else:
                peak_ref[part] = jnp.full((rows, 128), -1e30, jnp.float32)
        acc_ref[...] = jnp.zeros_like(acc_ref)

        def step(index, masked):
            at = pl.ds(pl.multiple_of(index * key_block, key_block), key_block)
            keys = kv_ref[at]
            values = ones_ref[at]
            for start in range(0, heads, HEADS_PER_DOT):
                part = pl.ds(start * rows, span)
                before = peak_ref[part]
                scores = lax.dot_general(
                    q_ref[r, part], keys, (((1,), (1,)), ((), ())),
                    preferred_element_type=jnp.float32,
                )
                if small:
                    scores = scores + jnp.concatenate([before] * (key_block // 128), axis=1)
                scores = scores.reshape(HEADS_PER_DOT, rows, key_block)
                scores = scores - decay_ref[index, start : start + HEADS_PER_DOT][:, None, :]
                if masked:
                    row = first + lax.broadcasted_iota(jnp.int32, (rows, key_block), 0)
                    col = index * key_block + lax.broadcasted_iota(
                        jnp.int32, (rows, key_block), 1
                    )
                    scores = jnp.where((col <= row)[None], scores, -1e30)
                scores = scores.reshape(span, key_block)
                if small:
                    weights = jnp.exp2(scores).astype(jnp.bfloat16)
                    acc_ref[part] += jnp.dot(weights, values, preferred_element_type=jnp.float32)
                else:
                    after = jnp.maximum(before, jnp.max(scores, axis=1, keepdims=True))
                    weights = jnp.exp2(scores - after[:, :1]).astype(jnp.bfloat16)
                    acc_ref[part] = acc_ref[part] * jnp.exp2(before - after) + jnp.dot(
                        weights, values, preferred_element_type=jnp.float32
                    )
                    peak_ref[part] = after

        full = first // key_block

        def body(index, carry):
            step(index, False)
            return carry

        lax.fori_loop(0, full, body, 0)
        step(full, True)
        for pair in range(heads // 2):
            even = acc_ref[(2 * pair) * rows : (2 * pair + 1) * rows]
            odd = acc_ref[(2 * pair + 1) * rows : (2 * pair + 2) * rows]
            done = jnp.where(low, pltpu.roll(even, 64, 1), odd) / jnp.where(
                low, even, pltpu.roll(odd, 64, 1)
            )
            out_ref[r, :, pair * 128 : (pair + 1) * 128] = done.astype(jnp.bfloat16)


def attend(place, near, far, row_decay, decays, kv, small):
    length = kv.shape[0]
    rows, width = near.shape
    heads, key_block = decays.shape[1:]
    vmem = pl.BlockSpec(memory_space=pltpu.VMEM)
    return pl.pallas_call(
        lambda *refs: attend_kernel(
            *refs, rows=rows, heads=heads, key_block=key_block, small=small
        ),
        out_shape=jax.ShapeDtypeStruct((2, rows, width), jnp.bfloat16),
        in_specs=[pl.BlockSpec(memory_space=pltpu.SMEM)] + [vmem] * 5,
        out_specs=vmem,
        scratch_shapes=[
            pltpu.VMEM((length, 128), jnp.bfloat16),
            pltpu.VMEM((2, heads * rows, 128), jnp.bfloat16),
            pltpu.VMEM((heads * rows, 128), jnp.float32),
            pltpu.VMEM((heads * rows, 128), jnp.float32),
        ],
        compiler_params=pltpu.CompilerParams(vmem_limit_bytes=40 * 1024 * 1024),
        name="attend_small" if small else "attend_any",
    )(place, near, far, row_decay, decays, kv)


def per_device(inputs, in_gain, w_query, w_key, w_value, query_gain, key_gain, decay_sums, w_out):
    sp_count = lax.axis_size("sp")
    kv_heads = lax.axis_size("kv")
    half_count = lax.axis_size("half")
    tp_count = kv_heads * half_count
    group = lax.axis_index("kv")
    me = (lax.axis_index("sp") * kv_heads + group) * half_count + lax.axis_index("half")
    count = sp_count * tp_count
    mirror = [(i, count - 1 - i) for i in range(count)]
    head_size = query_gain.shape[0]
    rows = inputs.shape[0]
    length = rows * count
    all_heads = w_query.shape[1] // head_size
    heads = all_heads // kv_heads
    width = heads * head_size
    members = sp_count * half_count
    key_block = math.gcd(length, KEY_BLOCK)

    def choose(a, b):
        return jnp.where(group == 0, a, b)

    normed = rms_norm(inputs.astype(jnp.float32), in_gain).astype(jnp.bfloat16)
    keys = rms_norm(
        jnp.dot(normed, w_key, preferred_element_type=jnp.float32).reshape(
            rows, kv_heads, head_size
        ),
        key_gain,
    ).astype(jnp.bfloat16)
    values = (
        jnp.dot(normed, w_value, preferred_element_type=jnp.float32)
        .astype(jnp.bfloat16)
        .reshape(rows, kv_heads, head_size)
    )
    pairs = jnp.concatenate([keys, values], axis=2)
    kv_blocks = pairs.transpose(1, 0, 2)
    decay_rows = (decay_sums.T * LOG2E).reshape(-1, 128)

    queries = rms_norm(
        jnp.dot(normed, w_query, preferred_element_type=jnp.float32).reshape(
            rows, all_heads, head_size
        ),
        query_gain * (LOG2E * head_size ** (-0.5)),
    ).astype(jnp.bfloat16).reshape(rows, kv_heads * width)
    own_q = choose(queries[:, :width], queries[:, width:])
    sent_q = choose(queries[:, width:], queries[:, :width])
    vmem = pl.BlockSpec(memory_space=pltpu.VMEM)
    chips = count // 2
    dma = pltpu.SemaphoreType.DMA
    kv, far_q, decay_all = pl.pallas_call(
        lambda *refs: exchange_kernel(
            *refs, rows=rows, sizes=(sp_count, kv_heads, half_count)
        ),
        out_shape=(
            jax.ShapeDtypeStruct((length, 128), jnp.bfloat16),
            jax.ShapeDtypeStruct((rows, width), jnp.bfloat16),
            jax.ShapeDtypeStruct((members, *decay_rows.shape), jnp.float32),
        ),
        in_specs=[vmem] * 3,
        out_specs=(vmem,) * 3,
        scratch_shapes=[
            dma((2,)), dma((chips,)), dma((count,)), dma((chips,)), dma((members // 2,)),
            dma((members,)), dma((members // 2,)), dma, dma,
        ],
        compiler_params=pltpu.CompilerParams(has_side_effects=True),
        name="exchange",
    )(kv_blocks, sent_q, decay_rows)
    decay_all = decay_all.reshape(sp_count, heads, -1, key_block)
    decay_all = decay_all.transpose(0, 2, 1, 3).reshape(length // key_block, heads, key_block)
    firsts = (me * rows, (count - 1 - me) * rows)
    place = jnp.stack(firsts).astype(jnp.int32)
    row_decay = jnp.stack(
        [
            lax.dynamic_slice(
                decay_all, (first // key_block, 0, first % key_block), (1, heads, rows)
            )[0].T
            for first in firsts
        ]
    )
    bound = head_size**0.5 * LOG2E * jnp.max(query_gain[:, None] * key_gain)
    near, far = [], []
    step = heads // 2 if heads % 4 == 0 else heads
    for start in range(0, heads, step):
        cols = slice(start * head_size, (start + step) * head_size)
        some = slice(start, start + step)
        attended = lax.cond(
            bound <= SMALL,
            lambda *given: attend(*given, True),
            lambda *given: attend(*given, False),
            place, own_q[:, cols], far_q[:, cols], row_decay[:, :, some], decay_all[:, some], kv,
        )
        near.append(attended[0])
        far.append(lax.ppermute(attended[1], ALL, mirror))
    near, back = jnp.concatenate(near, axis=1), jnp.concatenate(far, axis=1)
    whole = choose(
        jnp.concatenate([near, back], axis=1), jnp.concatenate([back, near], axis=1)
    )
    return jnp.dot(whole, w_out, preferred_element_type=jnp.float32).astype(jnp.bfloat16)


def solution(mesh):
    sp_count, tp_count = mesh.devices.shape
    split = Mesh(mesh.devices.reshape(sp_count, 2, tp_count // 2), ALL)
    placed = (P(ALL, None), P(), P(), P(), P(), P(), P(), P("sp", ("kv", "half")), P())
    return jax.shard_map(
        per_device, mesh=split, in_specs=placed, out_specs=P(ALL, None), check_vma=False
    )
```
